256 devices in a mesh: ep: 64 (over z, y, core), tp: 4 (over x).
Axes of the slice: x: 4, y: 4, z: 8, core: 2. Of those that a mesh axis runs over, the one named last changes fastest.
Arguments:
- queries_a: bfloat16 [8192, 1024], P('ep', 'tp'), may hold values from -128 to 128
- queries_b: bfloat16 [8192, 1024], P('ep', 'tp'), may hold values from -128 to 128
- keys_a: bfloat16 [8192, 512], P('ep', 'tp'), may hold values from -8 to 8
- keys_b: bfloat16 [8192, 512], P('ep', 'tp'), may hold values from -8 to 8
- values: bfloat16 [8192, 1024], P('ep', 'tp'), may hold values from -6 to 6
- lambdas: float32 [16], P('tp'), may hold values from 0.3 to 0.8
- head_gain: float32 [128], replicated, may hold values from 0.1 to 1.9
- w_out: bfloat16 [2048, 2048], P('tp'), may hold values from -0.125 to 0.125
- moe_tokens: bfloat16 [32768, 2048], P(('ep', 'tp')), may hold values from -80 to 80
- moe_gain: float32 [2048], replicated, may hold values from 0.1 to 1.9
- routes: int32 [32768, 2], P(('ep', 'tp')), may hold values from 0 to 63, all different within a row; in each aligned block of 128 rows (0 to 127, 128 to 255, ...) at most 6 rows name the same one
- route_weights: float32 [32768, 2], P(('ep', 'tp')), may hold values from 0.1 to 1
- w_gate: bfloat16 [64, 2048, 2048], P('ep', None, 'tp'), may hold values from -4 to 4
- w_up: bfloat16 [64, 2048, 2048], P('ep', None, 'tp'), may hold values from -4 to 4
- w_down: bfloat16 [64, 2048, 2048], P('ep', 'tp'), may hold values from -0.0625 to 0.0625
Outputs:
- mixer_out: bfloat16 [8192, 2048], P(('ep', 'tp'))
- moe_out: bfloat16 [32768, 2048], P(('ep', 'tp'))
The draws below stay inside these ranges and needn't reach their ends.
Inputs may be any that keep to these rules, and one draw needn't show every extreme that they name: `routes`: each row names 2 different experts. Within the rows of one device no expert is named by more than 6 rows, a bound that some block reaches of some device.
All inputs are finite; a program needn't handle non-finite values.
Results may differ from the reference program's by a relative error of at most 0.011.
Values may be sent and summed in bfloat16 or wider, within the bound.
No kernel may reach another device: no remote copies, remote signals or barrier semaphores. Data moves between devices by JAX's collectives and lax.ppermute only.
A program may use at most 192 MiB of HBM per device.

```python
import math
import jax
import jax.numpy as jnp
import numpy as np
from jax import lax

D = 2048
HEADS = 16
KV_HEADS = 8
HEAD = 64
VDIM = 128
FF = 2048
TOP = 2
ATT_DEV = 128
TOKB = 128
EXPERTS = 64
CAP = 6
SEQ = 8192
MOE_TOK = 32768
N_EP = 64
N_TP = 4


def query_key_pair(key, which):
    streams = jax.random.split(jax.random.fold_in(key, 1000 + which), 2)
    queries = 1.3 * jnp.clip(jax.random.normal(streams[0], (SEQ, HEADS * HEAD), jnp.float32), -4.0, 4.0)
    keys = 1.3 * jnp.clip(jax.random.normal(streams[1], (SEQ, KV_HEADS * HEAD), jnp.float32), -4.0, 4.0)
    return (queries, keys)


def draw_queries_a(key, part):
    return query_key_pair(key, 0)[0].astype(jnp.bfloat16)


def draw_keys_a(key, part):
    return query_key_pair(key, 0)[1].astype(jnp.bfloat16)


def draw_queries_b(key, part):
    return query_key_pair(key, 1)[0].astype(jnp.bfloat16)


def draw_keys_b(key, part):
    return query_key_pair(key, 1)[1].astype(jnp.bfloat16)


def draw_moe_tokens(key, part):
    streams = jax.random.split(jax.random.fold_in(key, 2000), 3)
    base = jnp.clip(jax.random.normal(streams[0], (MOE_TOK, D), jnp.float32), -4.0, 4.0)
    row_scale = jnp.exp(jax.random.uniform(streams[1], (MOE_TOK, 1), jnp.float32, math.log(0.3), math.log(3.0)))
    column_scale = jnp.exp(jax.random.uniform(streams[2], (1, D), jnp.float32, math.log(0.3), math.log(3.0)))
    result = base * row_scale * column_scale
    return result.astype(jnp.bfloat16)


def expert_matrix(key, salt):
    streams = jax.random.split(jax.random.fold_in(key, salt), 2)
    base = jnp.clip(jax.random.normal(streams[0], (EXPERTS, D, FF), jnp.float32), -4.0, 4.0) / math.sqrt(D)
    spread = jax.random.uniform(streams[1], (EXPERTS, 1, FF), jnp.float32, math.log(0.3), math.log(4.0))
    return (base * jnp.exp(spread)).astype(jnp.bfloat16)


def draw_w_gate(key, part):
    return expert_matrix(key, 3000)


def draw_w_up(key, part):
    return expert_matrix(key, 4000)


def block_scale(stream_key, extent, cuts, least, high):
    gain, own = 1.0, jax.random.fold_in(stream_key, 6)
    for position, parts in cuts:
        heights = jnp.exp(jax.random.uniform(jax.random.fold_in(own, position), (parts,), jnp.float32, least / len(cuts), high / len(cuts)))
        gain = gain * jnp.repeat(heights, extent[position] // parts).reshape([-1 if axis == position else 1 for axis in range(len(extent))])
    return gain


def deal_out(stream_key, own, number, rows, number_of, top, limit, skew):
    sequence = jax.random.permutation(stream_key, number_of)
    heavy_load, ordinary = shares(number_of, rows * top, limit, skew, True), shares(number_of, rows * top, limit, skew, False)
    places = jnp.arange(number_of)

    def named(tallies, offset_by):
        used = int((tallies > 0).sum())
        fixed = max(1, used // 4)
        shifted = fixed + (places - fixed + offset_by * (used - fixed)) % max(1, number_of - fixed)
        return jnp.zeros((number_of,), jnp.int32).at[sequence[jnp.where(places < fixed, places, shifted)]].set(jnp.asarray(tallies, jnp.int32))

    tallies = jnp.where(number % 4 == 0, named(heavy_load, number // 4), named(ordinary, number - number // 4 - 1))
    mixed = jax.random.permutation(jax.random.fold_in(own, 3), number_of)
    source_of, taker = mixed[0:number_of // 2 * 2:2], mixed[1:number_of // 2 * 2:2]
    slack = jnp.minimum(tallies[source_of] - 1, limit - tallies[taker]) // 2
    slack = jnp.where((source_of == sequence[0]) | (taker == sequence[0]) | (tallies[taker] == 0), 0, jnp.maximum(slack, 0))
    shifted = jax.random.randint(jax.random.fold_in(own, 4), (number_of // 2,), 0, 1 << 20) % (slack + 1)
    tallies = tallies.at[source_of].add(-shifted).at[taker].add(shifted)
    items = jnp.searchsorted(jnp.cumsum(tallies), jnp.arange(rows * top), side="right").astype(jnp.int32)
    grid = items.reshape(top, rows).T
    grid = grid[jax.random.permutation(jax.random.fold_in(own, 1), rows)]
    offset_by = jax.random.randint(jax.random.fold_in(own, 2), (rows, 1), 0, top)
    return jnp.take_along_axis(grid, (jnp.arange(top)[None, :] + offset_by) % top, axis=1)


def shares(number_of, total, most, slope, full):
    weights = [(1 << 20) // math.isqrt(rank ** slope) + 1 for rank in range(1, number_of + 1)]
    largest = most if full else min(most, max(-(-total // number_of), total * weights[0] // sum(weights)))
    least = 1 if total - largest >= number_of - 1 else 0
    given, rest = [largest] + [least] * (number_of - 1), total - largest - least * (number_of - 1)
    while rest > 0:
        free = [i for i in range(1, number_of) if given[i] < largest] or [i for i in range(1, number_of) if given[i] < most]
        whole, remaining = sum([weights[i] for i in free]), rest
        for i in free:
            addition = min(most - given[i], max(1, remaining * weights[i] // whole), rest)
            given[i] = given[i] + addition
            rest = rest - addition
    return np.array(given)


def bell_draw(key, shape, deviation, limit, shards=(), held_as=jnp.bfloat16):
    drawn = deviation * jax.random.normal(key, shape, jnp.float32)
    if shards:
        drawn = drawn * block_scale(key, shape, shards, -0.22, 0.18)
    return jnp.clip(drawn, -limit, limit).astype(held_as)


def setup_inputs(seed: int = 0) -> dict:
    key_list = jax.random.split(jax.random.key(seed), 16)
    queries_a = draw_queries_a(jax.random.fold_in(key_list[15], 71), 0)
    queries_b = draw_queries_b(jax.random.fold_in(key_list[15], 71), 0)
    keys_a = draw_keys_a(jax.random.fold_in(key_list[15], 71), 0)
    keys_b = draw_keys_b(jax.random.fold_in(key_list[15], 71), 0)
    values = bell_draw(key_list[4], (SEQ, KV_HEADS * VDIM), 1.0, 6.0, ((0, 64), (1, 4)))
    lambdas = jnp.clip(0.3 + 0.5 * jax.random.uniform(key_list[5], (HEADS,), jnp.float32) ** block_scale(key_list[5], (HEADS,), ((0, 4),), -0.2, 0.2), 0.3, 0.8)
    head_gain = jnp.clip(1.0 + 0.18 * jax.random.normal(key_list[6], (VDIM,), jnp.float32), 0.1, 1.9)
    w_out = bell_draw(key_list[7], (HEADS * VDIM, D), (HEADS * VDIM) ** -0.5, 0.125, ((0, 4),))
    moe_tokens = draw_moe_tokens(jax.random.fold_in(key_list[15], 71), 0)
    moe_gain = jnp.clip(1.0 + 0.18 * jax.random.normal(key_list[9], (D,), jnp.float32), 0.1, 1.9)
    routes_keys = jax.random.split(jax.random.fold_in(key_list[10], 1), MOE_TOK // TOKB)
    routes_turns = jax.random.permutation(jax.random.fold_in(key_list[10], 3), MOE_TOK // TOKB)
    routes = jax.vmap(lambda own, number: deal_out(jax.random.fold_in(key_list[10], 2), own, number, TOKB, EXPERTS, TOP, CAP, 2))(routes_keys, routes_turns).reshape((MOE_TOK, TOP))
    route_weights = jnp.clip(0.1 + 0.9 * jax.random.uniform(key_list[11], (MOE_TOK, TOP), jnp.float32) ** block_scale(key_list[11], (MOE_TOK, TOP), ((0, 256),), -0.2, 0.2), 0.1, 1.0)
    w_gate = draw_w_gate(jax.random.fold_in(key_list[15], 71), 0)
    w_up = draw_w_up(jax.random.fold_in(key_list[15], 71), 0)
    w_down = bell_draw(key_list[14], (EXPERTS, FF, D), (4 * FF) ** -0.5, 0.0625, ((0, 64), (1, 4)))
    return {"queries_a": queries_a, "queries_b": queries_b, "keys_a": keys_a, "keys_b": keys_b, "values": values, "lambdas": lambdas, "head_gain": head_gain, "w_out": w_out, "moe_tokens": moe_tokens, "moe_gain": moe_gain, "routes": routes, "route_weights": route_weights, "w_gate": w_gate, "w_up": w_up, "w_down": w_down}


eps = 1e-05
alpha_act = 1.702
limit_act = 7.0

def clamped_unit(gate, up):
    capped = jnp.minimum(gate, limit_act)
    linear = jnp.clip(up, -limit_act, limit_act)
    return capped * jax.nn.sigmoid(alpha_act * capped) * (linear + 1.0)

def hidden_rows(inputs, gate_matrix, up_matrix):
    gate = jnp.dot(inputs, gate_matrix, preferred_element_type=jnp.float32)
    up = jnp.dot(inputs, up_matrix, preferred_element_type=jnp.float32)
    return clamped_unit(gate, up).astype(jnp.bfloat16)

def map_weights(queries, keys, value_rows, query_pos, key_pos):
    scores = jnp.dot(queries, keys.T, preferred_element_type=jnp.float32) * HEAD ** (-0.5)
    visible = key_pos[None, :] <= query_pos[:, None]
    scores = jnp.where(visible, scores, -jnp.inf)
    peak = lax.optimization_barrier(jnp.max(scores, axis=1, keepdims=True))
    expo = jnp.where(visible, jnp.exp(scores - peak), 0.0)
    total = lax.optimization_barrier(jnp.sum(expo, axis=1, keepdims=True))
    mixed = jnp.dot(expo.astype(jnp.bfloat16), value_rows, preferred_element_type=jnp.float32)
    return mixed / total

def one_head(head, queries_a, queries_b, keys_a, keys_b, values, lambdas, head_gain):
    kv_head = head // (HEADS // KV_HEADS)
    query_a = lax.dynamic_slice_in_dim(queries_a, (head * HEAD).astype(jnp.int32), HEAD, 1)
    query_b = lax.dynamic_slice_in_dim(queries_b, (head * HEAD).astype(jnp.int32), HEAD, 1)
    key_a = lax.dynamic_slice_in_dim(keys_a, (kv_head * HEAD).astype(jnp.int32), HEAD, 1)
    key_b = lax.dynamic_slice_in_dim(keys_b, (kv_head * HEAD).astype(jnp.int32), HEAD, 1)
    value_head = lax.dynamic_slice_in_dim(values, (kv_head * VDIM).astype(jnp.int32), VDIM, 1)
    key_pos = jnp.arange(SEQ, dtype=jnp.int32)
    strength = lambdas[head]

    def one_block(index):
        start = (index * ATT_DEV).astype(jnp.int32)
        query_pos = start + jnp.arange(ATT_DEV, dtype=jnp.int32)
        first = map_weights(lax.dynamic_slice_in_dim(query_a, start, ATT_DEV, 0), key_a, value_head, query_pos, key_pos)
        second = map_weights(lax.dynamic_slice_in_dim(query_b, start, ATT_DEV, 0), key_b, value_head, query_pos, key_pos)
        diff = first - strength * second
        scaled = diff * lax.rsqrt(lax.optimization_barrier(jnp.mean(diff * diff, axis=-1, keepdims=True)) + eps) * head_gain
        return scaled.astype(jnp.bfloat16)
    return lax.map(one_block, jnp.arange(N_EP, dtype=jnp.int32)).reshape(SEQ, VDIM)

def reference(queries_a, queries_b, keys_a, keys_b, values, lambdas, head_gain, w_out, moe_tokens, moe_gain, routes, route_weights, w_gate, w_up, w_down):
    heads = lax.map(lambda head: one_head(head, queries_a, queries_b, keys_a, keys_b, values, lambdas, head_gain), jnp.arange(HEADS, dtype=jnp.int32))
    heads = heads.transpose(1, 0, 2).reshape(SEQ, N_TP, HEADS // N_TP * VDIM)
    weight_groups = w_out.reshape(N_TP, HEADS // N_TP * VDIM, D)
    head_parts = jnp.einsum('sjc,jcd->jsd', heads.astype(jnp.float32), weight_groups.astype(jnp.float32))
    head_parts = lax.optimization_barrier(head_parts.astype(jnp.bfloat16))
    mixer_out = lax.optimization_barrier(jnp.sum(head_parts.astype(jnp.float32), axis=0)).astype(jnp.bfloat16)
    inputs = moe_tokens.astype(jnp.float32)
    normed = (inputs * lax.rsqrt(lax.optimization_barrier(jnp.mean(inputs * inputs, axis=-1, keepdims=True)) + eps) * moe_gain).astype(jnp.bfloat16)
    blocks = MOE_TOK // TOKB
    chosen = routes.reshape(blocks, TOKB * TOP)
    member = (chosen[:, :, None] == jnp.arange(EXPERTS, dtype=jnp.int32)[None, None, :]).astype(jnp.int32)
    order_in = lax.optimization_barrier(jnp.sum(jnp.cumsum(member, axis=1) * member, axis=2)) - 1
    block_ids = jnp.arange(blocks, dtype=jnp.int32)[:, None]
    slot_ids = ((chosen * blocks + block_ids) * CAP + order_in).astype(jnp.int32)
    token_ids = (block_ids * TOKB + jnp.arange(TOKB * TOP, dtype=jnp.int32)[None, :] // TOP).astype(jnp.int32)
    owner = jnp.full((EXPERTS * blocks * CAP,), MOE_TOK, jnp.int32).at[slot_ids.reshape(-1)].set(token_ids.reshape(-1))
    owner = owner.reshape(EXPERTS, blocks * CAP)

    def one_expert(index):
        slot_owner = owner[index]
        valid = slot_owner < MOE_TOK
        taken = jnp.take(normed, jnp.minimum(slot_owner, MOE_TOK - 1), axis=0)
        taken = jnp.where(valid[:, None], taken, jnp.zeros_like(taken))
        hidden = hidden_rows(taken, w_gate[index], w_up[index])
        unit_parts = jnp.einsum('rjf,jfd->jrd', hidden.reshape(-1, N_TP, FF // N_TP).astype(jnp.float32), w_down[index].reshape(N_TP, FF // N_TP, D).astype(jnp.float32))
        unit_parts = lax.optimization_barrier(unit_parts.astype(jnp.bfloat16))
        return lax.optimization_barrier(jnp.sum(unit_parts.astype(jnp.float32), axis=0)).astype(jnp.bfloat16)
    expert_rows = lax.map(one_expert, jnp.arange(EXPERTS, dtype=jnp.int32))
    picked = jnp.take(expert_rows.reshape(-1, D), slot_ids.reshape(-1), axis=0).reshape(MOE_TOK, TOP, D)
    moe_out = lax.optimization_barrier(jnp.sum(picked.astype(jnp.float32) * route_weights[:, :, None], axis=1)).astype(jnp.bfloat16)
    return (mixer_out, moe_out)
```

```python
import jax
import jax.numpy as jnp
from jax import lax
from jax.experimental import pallas as pl
from jax.experimental.pallas import tpu as pltpu
from jax.sharding import PartitionSpec as P

HEAD = 64
VDIM = 128
TOP = 2
EXPERTS = 64
WIDTH = 2048
BLOCK = 256
PART = 2
CHUNKS = 3

eps = 1e-05
alpha_act = 1.702
limit_act = 7.0
negative = -1e30
log2e = 1.4426950408889634


def ring(shift):
    return [(i, (i + shift) % 4) for i in range(4)]


def z_swap(bit):
    return [(i, i ^ (bit * 8)) for i in range(64)]


def y_shift(shift):
    return [(i, (i // 8) * 8 + ((i // 2 + shift) % 4) * 2 + i % 2) for i in range(64)]


core_swap = [(i, i ^ 1) for i in range(64)]


def dispatch_kernel(tokens_ref, gain_ref, routes_ref, *outs):
    pos_ref, parts = outs[0], outs[1:]
    rows = tokens_ref.shape[0]
    inputs = tokens_ref[...].astype(jnp.float32)
    normed = (
        inputs * lax.rsqrt(jnp.mean(inputs * inputs, axis=-1, keepdims=True) + eps) * gain_ref[...]
    ).astype(jnp.bfloat16)
    expert = lax.broadcasted_iota(jnp.int32, (rows, 128), 1)
    first = routes_ref[:, 0:1]
    second = routes_ref[:, 1:2]
    is_first = (expert == first).astype(jnp.float32)
    is_second = (expert == second).astype(jnp.float32)
    member = is_first + is_second
    before = (
        lax.broadcasted_iota(jnp.int32, (rows, rows), 1)
        < lax.broadcasted_iota(jnp.int32, (rows, rows), 0)
    ).astype(jnp.bfloat16)
    count = jnp.dot(before, member.astype(jnp.bfloat16), preferred_element_type=jnp.float32)

    def place(chosen, route):
        order = jnp.sum(count * chosen, axis=1, keepdims=True).astype(jnp.int32)
        chunk = (order >= 2).astype(jnp.int32) + (order >= 4).astype(jnp.int32)
        return chunk * (EXPERTS * PART) + route * PART + (order - 2 * chunk)

    pos = (place(is_first, first), place(is_second, second))
    pos_ref[:, 0:1] = pos[0]
    pos_ref[:, 1:2] = pos[1]
    slot = lax.broadcasted_iota(jnp.int32, (rows, EXPERTS * PART), 1)
    for k, out_ref in enumerate(parts):
        here = slot + k * EXPERTS * PART
        chosen = ((here == pos[0]) | (here == pos[1])).astype(jnp.float32).astype(jnp.bfloat16)
        out_ref[...] = lax.dot_general(
            chosen, normed, (((0,), (0,)), ((), ())), preferred_element_type=jnp.float32
        ).astype(jnp.bfloat16)


def combine_kernel(pos_ref, weights_ref, *refs):
    parts, out_ref = refs[:-1], refs[-1]
    rows = out_ref.shape[0]
    slot = lax.broadcasted_iota(jnp.int32, (rows, EXPERTS * PART), 1)
    total = jnp.zeros(out_ref.shape, jnp.float32)
    for k, part_ref in enumerate(parts):
        here = slot + k * EXPERTS * PART
        mix = jnp.where(here == pos_ref[:, 0:1], weights_ref[:, 0:1], 0.0) + jnp.where(
            here == pos_ref[:, 1:2], weights_ref[:, 1:2], 0.0
        )
        high = mix.astype(jnp.bfloat16)
        low = (mix - high.astype(jnp.float32)).astype(jnp.bfloat16)
        table = part_ref[...]
        total = total + jnp.dot(high, table, preferred_element_type=jnp.float32)
        total = total + jnp.dot(low, table, preferred_element_type=jnp.float32)
    out_ref[...] = total.astype(jnp.bfloat16)


def clamped_unit(gate, up):
    capped = jnp.minimum(gate, limit_act)
    linear = jnp.clip(up, -limit_act, limit_act)
    return capped * jax.nn.sigmoid(alpha_act * capped) * (linear + 1.0)


def feed_forward(rows, w_gate, w_up, w_down):
    gate = jnp.dot(rows, w_gate, preferred_element_type=jnp.float32)
    up = jnp.dot(rows, w_up, preferred_element_type=jnp.float32)
    hidden = clamped_unit(gate, up).astype(jnp.bfloat16)
    return jnp.dot(hidden, w_down, preferred_element_type=jnp.float32).astype(jnp.bfloat16)


def gather_tp(mine):
    half = mine.shape[0] // 2
    left = lax.ppermute(mine, "tp", ring(1))
    right = lax.ppermute(mine, "tp", ring(-1))
    far_a = lax.ppermute(left[:half], "tp", ring(1))
    far_b = lax.ppermute(right[half:], "tp", ring(-1))
    return jnp.concatenate([mine, left, right, far_a, far_b], axis=0)


def plus(a, b):
    return (a.astype(jnp.float32) + b.astype(jnp.float32)).astype(jnp.bfloat16)


def scatter_tp(pieces):
    own, to_left, to_right, far = pieces
    half = own.shape[0] // 2
    from_left = lax.ppermute(far[:half], "tp", ring(1))
    from_right = lax.ppermute(far[half:], "tp", ring(-1))
    going_right = jnp.concatenate([plus(to_right[:half], from_left), to_right[half:]], axis=0)
    going_left = jnp.concatenate([to_left[:half], plus(to_left[half:], from_right)], axis=0)
    a = lax.ppermute(going_right, "tp", ring(1))
    b = lax.ppermute(going_left, "tp", ring(-1))
    return (
        own.astype(jnp.float32) + a.astype(jnp.float32) + b.astype(jnp.float32)
    ).astype(jnp.bfloat16)


def exchange(part):
    swapped = lax.all_to_all(part.reshape(EXPERTS, PART, WIDTH), "ep", 0, 0, tiled=True)
    return swapped


def attention_kernel(place_ref, lambdas_ref, q_ref, kv_ref, gain_ref, out_ref, peak, total, accum):
    own = place_ref[0]
    core = place_ref[1]
    own_z = own // 4
    own_y = own % 4
    rows = q_ref.shape[0]
    tiles = rows // BLOCK
    peak[...] = jnp.full(peak.shape, negative, jnp.float32)
    total[...] = jnp.zeros(total.shape, jnp.float32)
    accum[...] = jnp.zeros(accum.shape, jnp.float32)

    def start_of(chip):
        differ = (chip // 4) ^ own_z
        deep = ((differ >> 2) & 1) + (differ & 2) + ((differ & 1) << 2)
        step = (chip + 4 - own_y) % 4
        side = jnp.where(step == 3, 1, jnp.where(step == 0, 0, step + 1))
        return pl.multiple_of((side * 8 + deep) * BLOCK, BLOCK)

    def visit(pair, masked):
        near = start_of(2 * pair)
        next_ = start_of(2 * pair + 1)
        keys = jnp.concatenate(
            [kv_ref[pl.ds(near, BLOCK), : 2 * HEAD], kv_ref[pl.ds(next_, BLOCK), : 2 * HEAD]], axis=0
        )
        vals = jnp.concatenate(
            [kv_ref[pl.ds(near, BLOCK), 2 * HEAD :], kv_ref[pl.ds(next_, BLOCK), 2 * HEAD :]], axis=0
        )
        for t in range(tiles):
            at = pl.ds(t * BLOCK, BLOCK)
            scores = lax.dot_general(
                q_ref[at, :], keys, (((1,), (1,)), ((), ())), preferred_element_type=jnp.float32
            ) * (HEAD ** (-0.5) * log2e)
            if masked:
                key_pos = 2 * pair * BLOCK + lax.broadcasted_iota(jnp.int32, scores.shape, 1)
                query_pos = own * BLOCK + lax.broadcasted_iota(jnp.int32, scores.shape, 0)
                scores = jnp.where(key_pos <= query_pos, scores, negative)
            old = peak[at, :]
            new = jnp.maximum(old, jnp.max(scores, axis=1, keepdims=True))
            keep = jnp.exp2(old - new)
            expo = jnp.exp2(scores - new[:, :1])
            peak[at, :] = new
            total[at, :] = keep * total[at, :] + jnp.sum(expo, axis=1, keepdims=True)
            accum[at, :] = keep * accum[at, :] + jnp.dot(
                expo.astype(jnp.bfloat16), vals, preferred_element_type=jnp.float32
            )

    def step(pair, carry):
        visit(pair, False)
        return carry

    lax.fori_loop(0, own // 2, step, 0)
    visit(own // 2, True)
    for h in range(tiles // 2):
        at = pl.ds(h * BLOCK, BLOCK)
        bt = pl.ds((tiles // 2 + h) * BLOCK, BLOCK)
        strength = lambdas_ref[core * (tiles // 2) + h]
        diff = accum[at, :] / total[at, :] - strength * (accum[bt, :] / total[bt, :])
        normal = diff * lax.rsqrt(jnp.mean(diff * diff, axis=1, keepdims=True) + eps)
        out_ref[:, h * VDIM : (h + 1) * VDIM] = (normal * gain_ref[...]).astype(jnp.bfloat16)


def attend(place, lambdas, q, kv, gain):
    rows = q.shape[0]
    return pl.pallas_call(
        attention_kernel,
        out_shape=jax.ShapeDtypeStruct((BLOCK, 2 * VDIM), jnp.bfloat16),
        in_specs=[
            pl.BlockSpec(memory_space=pltpu.SMEM),
            pl.BlockSpec(memory_space=pltpu.SMEM),
            pl.BlockSpec(memory_space=pltpu.VMEM),
            pl.BlockSpec(memory_space=pltpu.VMEM),
            pl.BlockSpec(memory_space=pltpu.VMEM),
        ],
        out_specs=pl.BlockSpec(memory_space=pltpu.VMEM),
        scratch_shapes=[
            pltpu.VMEM((rows, VDIM), jnp.float32),
            pltpu.VMEM((rows, VDIM), jnp.float32),
            pltpu.VMEM((rows, VDIM), jnp.float32),
        ],
        compiler_params=pltpu.CompilerParams(vmem_limit_bytes=40 * 1024 * 1024),
        cost_estimate=pl.CostEstimate(
            flops=6_000_000_000, transcendentals=8_000_000, bytes_accessed=5_000_000
        ),
        name="attention",
    )(place, lambdas, q, kv, gain)


def swap_heads(queries_a, queries_b, keys_a, keys_b, values):
    core = lax.axis_index("ep") % 2

    def columns(g):
        return jnp.concatenate(
            [
                keys_a[:, g * HEAD : (g + 1) * HEAD],
                keys_b[:, g * HEAD : (g + 1) * HEAD],
                values[:, g * VDIM : (g + 1) * VDIM],
                queries_a[:, g * 2 * HEAD : (g + 1) * 2 * HEAD],
                queries_b[:, g * 2 * HEAD : (g + 1) * 2 * HEAD],
            ],
            axis=1,
        )

    zero, one = columns(0), columns(1)
    mine = jnp.where(core == 0, zero, one)
    other = lax.ppermute(jnp.where(core == 0, one, zero), "ep", core_swap)
    both = jnp.concatenate(
        [jnp.where(core == 0, mine, other), jnp.where(core == 0, other, mine)], axis=0
    )
    return both[:, :256], both[:, 256:]


def gather_kv(kv):
    for bit in (4, 2, 1):
        kv = jnp.concatenate([kv, lax.ppermute(kv, "ep", z_swap(bit))], axis=0)
    return jnp.concatenate([kv] + [lax.ppermute(kv, "ep", y_shift(s)) for s in (1, -1, 2)], axis=0)


def body(
    queries_a,
    queries_b,
    keys_a,
    keys_b,
    values,
    lambdas,
    head_gain,
    w_out,
    moe_tokens,
    moe_gain,
    routes,
    route_weights,
    w_gate,
    w_up,
    w_down,
):
    rows, width = moe_tokens.shape
    core = lax.axis_index("ep") % 2
    part_shape = jax.ShapeDtypeStruct((EXPERTS * PART, width), jnp.bfloat16)
    pos, *parts = pl.pallas_call(
        dispatch_kernel,
        out_shape=[jax.ShapeDtypeStruct((rows, TOP), jnp.int32)] + [part_shape] * CHUNKS,
        name="dispatch",
    )(moe_tokens, moe_gain.reshape(1, width), routes)
    arrived = [exchange(part) for part in parts]

    kv, q = swap_heads(queries_a, queries_b, keys_a, keys_b, values)
    none = jnp.zeros((BLOCK, HEAD), jnp.bfloat16)
    q_rows = jnp.concatenate(
        [jnp.concatenate([q[:, h * HEAD : (h + 1) * HEAD], none], axis=1) for h in (0, 1)]
        + [jnp.concatenate([none, q[:, h * HEAD : (h + 1) * HEAD]], axis=1) for h in (2, 3)],
        axis=0,
    )
    place = jnp.stack([lax.axis_index("ep") // 2, core]).astype(jnp.int32)

    returned = []
    for part in arrived:
        table = gather_tp(part).reshape(-1, width)
        outs = feed_forward(table, w_gate[0], w_up[0], w_down[0])
        size = EXPERTS * PART
        owned = scatter_tp([outs[j * size : (j + 1) * size] for j in range(4)])
        returned.append(exchange(owned).reshape(size, width))

    heads = attend(place, lambdas, q_rows, gather_kv(kv), head_gain.reshape(1, VDIM))
    low, high = heads[: BLOCK // 2], heads[BLOCK // 2 :]
    mine = jnp.where(core == 0, low, high)
    other = lax.ppermute(jnp.where(core == 0, high, low), "ep", core_swap)
    heads_out = jnp.concatenate(
        [jnp.where(core == 0, mine, other), jnp.where(core == 0, other, mine)], axis=1
    )
    partial = jnp.dot(heads_out, w_out, preferred_element_type=jnp.float32).astype(jnp.bfloat16)
    tp = lax.axis_index("tp")
    share = partial.shape[0] // 4
    piece = lambda s: lax.dynamic_slice_in_dim(partial, ((tp + s) % 4) * share, share, 0)
    mixer_sum = piece(0).astype(jnp.float32)
    for s in (1, -1, 2):
        mixer_sum = mixer_sum + lax.ppermute(piece(s % 4), "tp", ring(s)).astype(jnp.float32)
    mixer_out = mixer_sum.astype(jnp.bfloat16)

    moe_out = pl.pallas_call(
        combine_kernel,
        out_shape=jax.ShapeDtypeStruct((rows, width), jnp.bfloat16),
        name="combine",
    )(pos, route_weights, *returned)
    return (mixer_out, moe_out)


def solution(mesh):
    return jax.shard_map(
        body,
        mesh=mesh,
        in_specs=(
            P("ep", "tp"),
            P("ep", "tp"),
            P("ep", "tp"),
            P("ep", "tp"),
            P("ep", "tp"),
            P("tp"),
            P(),
            P("tp", None),
            P(("ep", "tp"), None),
            P(),
            P(("ep", "tp"), None),
            P(("ep", "tp"), None),
            P("ep", None, "tp"),
            P("ep", None, "tp"),
            P("ep", "tp", None),
        ),
        out_specs=(P(("ep", "tp"), None), P(("ep", "tp"), None)),
        check_vma=False,
    )
```
